32 devices in a mesh: grp: 2 (over x), ep: 8 (over z, y), tp: 2 (over core).
Axes of the slice: x: 2, y: 2, z: 4, core: 2. Of those that a mesh axis runs over, the one named last changes fastest.
Arguments:
- tokens: bfloat16 [3072, 2048], P(('grp', 'ep'), 'tp'), parts along dimension 0, may hold values from -10 to 10
- gain_in: float32 [2048], replicated, may hold values from 0.1 to 1.9
- gain_out: float32 [2048], replicated, may hold values from 0.1 to 1.9
- expert_ids: int32 [3072, 2], P(('grp', 'ep')), parts along dimension 0, may hold values from 0 to 3, all different within a row; in each aligned block of 192 rows (0 to 191, 192 to 383, ...) at most 144 rows name the same one
- route_weight: float32 [3072, 2], P(('grp', 'ep')), parts along dimension 0, may hold values from 0.1 to 1
- gate_weight: bfloat16 [8, 2048, 1792], P('ep', None, 'tp'), may hold values from -0.125 to 0.125
- up_weight: bfloat16 [8, 2048, 1792], P('ep', None, 'tp'), may hold values from -0.125 to 0.125
- down_weight: bfloat16 [8, 1792, 2048], P('ep', 'tp'), may hold values from -1 to 1
Outputs:
- layer_out: bfloat16 [3072, 2048], P(('grp', 'ep'), 'tp'), parts along dimension 0
The draws below stay inside these ranges and needn't reach their ends.
There are 2 independent parts, one for each index of `grp`. The reference program is written for one: setup_inputs(seed, part) draws one part's arguments, and reference() takes and returns one part's arrays. A program takes and returns all parts, laid end to end along the dimension named above; an argument that names none is the same for every part. Nothing has to cross between parts.
Inputs may be any that keep to these rules, and one draw needn't show every extreme that they name: `expert_ids`: each row names 2 different experts. Among the tokens of one index of ep no expert is named more than 144 times, a bound that some block reaches.
All inputs are finite; a program needn't handle non-finite values.
Results may differ from the reference program's by a relative error of at most 0.0077.
Values may be sent and summed in bfloat16 or wider, within the bound.
A program may use at most 64 MiB of HBM per device.

```python
import math
import jax
import jax.numpy as jnp
import numpy as np
from jax import lax

D = 2048
DE = 3584
TOP_K = 2
TOK_EP = 192
EXPERTS = 4
TOKENS = 1536
CAP = 144
N_EP = 8


def column_factors(key):
    key_low, key_high, key_flip = jax.random.split(jax.random.fold_in(key, 11), 3)
    lowest = jax.random.uniform(key_low, (), jnp.float32, 0.35, 0.55)
    highest = jax.random.uniform(key_high, (), jnp.float32, 1.7, 2.4)
    flipped = jax.random.randint(key_flip, (), 0, 2) == 1
    first_half = jnp.where(flipped, highest, lowest)
    second_half = jnp.where(flipped, lowest, highest)
    return jnp.concatenate([jnp.full((D // 2,), first_half, jnp.float32), jnp.full((D - D // 2,), second_half, jnp.float32)])


def draw_tokens(key, part):
    key_base, key_rows = jax.random.split(jax.random.fold_in(key, 3))
    base = jnp.clip(jax.random.normal(key_base, (TOKENS, D), jnp.float32), -4.0, 4.0)
    return (base * column_factors(jax.random.fold_in(key, 5))[None, :]).astype(jnp.bfloat16)


def draw_down_weight(key, part):
    key_base = jax.random.fold_in(key, 7)
    base = jnp.clip(jax.random.normal(key_base, (2 * EXPERTS, DE // 2, D), jnp.float32), -4.0, 4.0)
    base = base * DE ** (-0.5)
    return (base * column_factors(jax.random.fold_in(key, 9))[None, None, :]).astype(jnp.bfloat16)


def block_levels(rng, shape, pieces, low, top_value):
    factor_of, own = 1.0, jax.random.fold_in(rng, 6)
    for position, blocks in pieces:
        steps = jnp.exp(jax.random.uniform(jax.random.fold_in(own, position), (blocks,), jnp.float32, low / len(pieces), top_value / len(pieces)))
        factor_of = factor_of * jnp.repeat(steps, shape[position] // blocks).reshape([-1 if axis == position else 1 for axis in range(len(shape))])
    return factor_of


def routed_block(rng, own, number, rows, count, top, bound, slope):
    ranking = jax.random.permutation(rng, count)
    heavy_load, usual = portions_of(count, rows * top, bound, slope, True), portions_of(count, rows * top, bound, slope, False)
    places = jnp.arange(count)

    def named(sizes, offset_by):
        used = int((sizes > 0).sum())
        fixed = max(1, used // 4)
        moved = fixed + (places - fixed + offset_by * (used - fixed)) % max(1, count - fixed)
        return jnp.zeros((count,), jnp.int32).at[ranking[jnp.where(places < fixed, places, moved)]].set(jnp.asarray(sizes, jnp.int32))

    sizes = jnp.where(number % 4 == 0, named(heavy_load, number // 4), named(usual, number - number // 4 - 1))
    mixed = jax.random.permutation(jax.random.fold_in(own, 3), count)
    source_of, sink = mixed[0:count // 2 * 2:2], mixed[1:count // 2 * 2:2]
    room = jnp.minimum(sizes[source_of] - 1, bound - sizes[sink]) // 2
    room = jnp.where((source_of == ranking[0]) | (sink == ranking[0]) | (sizes[sink] == 0), 0, jnp.maximum(room, 0))
    moved = jax.random.randint(jax.random.fold_in(own, 4), (count // 2,), 0, 1 << 20) % (room + 1)
    sizes = sizes.at[source_of].add(-moved).at[sink].add(moved)
    labels = jnp.searchsorted(jnp.cumsum(sizes), jnp.arange(rows * top), side="right").astype(jnp.int32)
    table = labels.reshape(top, rows).T
    table = table[jax.random.permutation(jax.random.fold_in(own, 1), rows)]
    offset_by = jax.random.randint(jax.random.fold_in(own, 2), (rows, 1), 0, top)
    return jnp.take_along_axis(table, (jnp.arange(top)[None, :] + offset_by) % top, axis=1)


def portions_of(amount, total, bound, skew, full):
    weights = [(1 << 20) // math.isqrt(rank ** skew) + 1 for rank in range(1, amount + 1)]
    largest = bound if full else min(bound, max(-(-total // amount), total * weights[0] // sum(weights)))
    least = 1 if total - largest >= amount - 1 else 0
    counts, surplus = [largest] + [least] * (amount - 1), total - largest - least * (amount - 1)
    while surplus > 0:
        free = [i for i in range(1, amount) if counts[i] < largest] or [i for i in range(1, amount) if counts[i] < bound]
        pool, budget = sum([weights[i] for i in free]), surplus
        for i in free:
            more = min(bound - counts[i], max(1, budget * weights[i] // pool), surplus)
            counts[i] = counts[i] + more
            surplus = surplus - more
    return np.array(counts)


def scatter_about(rng, dims, deviation, limit, cuts=(), kind=jnp.bfloat16):
    result = jax.random.normal(rng, dims, jnp.float32) * deviation
    if len(cuts) > 0:
        result = block_levels(rng, dims, cuts, -0.22, 0.18) * result
    return jnp.clip(result, min=-limit, max=limit).astype(kind)


def setup_inputs(seed: int = 0, part: int = 0) -> dict:
    seeds = jax.random.split(jax.random.key(seed), 9)
    own_keys = jax.random.split(jax.random.fold_in(seeds[8], part), 9)
    tokens = draw_tokens(jax.random.fold_in(jax.random.fold_in(seeds[8], part), 71), part)
    gain_in = jnp.clip(1.0 + 0.18 * jax.random.normal(seeds[1], (D,), jnp.float32), 0.1, 1.9)
    gain_out = jnp.clip(1.0 + 0.18 * jax.random.normal(seeds[2], (D,), jnp.float32), 0.1, 1.9)
    expert_ids_keys = jax.random.split(jax.random.fold_in(own_keys[3], 1), TOKENS // TOK_EP)
    expert_ids_turns = jax.random.permutation(jax.random.fold_in(own_keys[3], 3), TOKENS // TOK_EP)
    expert_ids = jax.vmap(lambda own, number: routed_block(jax.random.fold_in(own_keys[3], 2), own, number, TOK_EP, EXPERTS, TOP_K, CAP, 2))(expert_ids_keys, expert_ids_turns).reshape((TOKENS, TOP_K))
    route_weight = jnp.clip(0.1 + 0.9 * jax.random.uniform(own_keys[4], (TOKENS, TOP_K), jnp.float32) ** block_levels(own_keys[4], (TOKENS, TOP_K), ((0, 8),), -0.2, 0.2), 0.1, 1.0)
    gate_weight = scatter_about(seeds[5], (2 * EXPERTS, D, DE // 2), D ** -0.5, 0.125, ((0, 8), (2, 2)))
    up_weight = scatter_about(seeds[6], (2 * EXPERTS, D, DE // 2), D ** -0.5, 0.125, ((0, 8), (2, 2)))
    down_weight = draw_down_weight(jax.random.fold_in(seeds[8], 71), part)
    return dict(tokens=tokens, gain_in=gain_in, gain_out=gain_out, expert_ids=expert_ids, route_weight=route_weight, gate_weight=gate_weight, up_weight=up_weight, down_weight=down_weight)


norm_eps = 1e-06

def expert_rows(items):
    gathered, gate_pair, up_pair, down_pair = items
    quarter = gate_pair.shape[2] // 2
    rows_float = gathered.astype(jnp.float32)
    total = jnp.zeros((gathered.shape[0], down_pair.shape[2]), jnp.float32)
    for which_half in range(2):
        summed = jnp.zeros((gathered.shape[0], down_pair.shape[2]), jnp.float32)
        for which_core in range(2):
            start_col = which_core * quarter
            gate_pre = jnp.dot(rows_float, gate_pair[which_half, :, start_col:start_col + quarter].astype(jnp.float32), precision=lax.Precision.HIGHEST)
            up_pre = jnp.dot(rows_float, up_pair[which_half, :, start_col:start_col + quarter].astype(jnp.float32), precision=lax.Precision.HIGHEST)
            hidden = (jax.nn.silu(gate_pre) * up_pre).astype(jnp.bfloat16)
            partial_value = jnp.dot(hidden.astype(jnp.float32), down_pair[which_half, start_col:start_col + quarter, :].astype(jnp.float32), precision=lax.Precision.HIGHEST)
            partial_value = lax.optimization_barrier(partial_value.astype(jnp.bfloat16)).astype(jnp.float32)
            summed = summed + partial_value
        total = total + lax.optimization_barrier(summed.astype(jnp.bfloat16)).astype(jnp.float32)
    return total

def reference(tokens, gain_in, gain_out, expert_ids, route_weight, gate_weight, up_weight, down_weight):
    xfloat = tokens.astype(jnp.float32)
    factor = lax.rsqrt(lax.optimization_barrier(jnp.mean(xfloat * xfloat, axis=1, keepdims=True)) + norm_eps)
    normed = (xfloat * factor * gain_in).astype(jnp.bfloat16)
    copies = TOK_EP * TOP_K
    flat_ids = expert_ids.reshape(N_EP, copies).astype(jnp.int32)
    onehot = (flat_ids[:, :, None] == jnp.arange(EXPERTS, dtype=jnp.int32)[None, None, :]).astype(jnp.int32)
    before = jnp.cumsum(onehot, axis=1) - onehot
    slots = lax.optimization_barrier(jnp.sum(before * onehot, axis=2)).astype(jnp.int32)
    targets = (flat_ids * CAP + slots).astype(jnp.int32)
    source = (jnp.arange(copies, dtype=jnp.int32) // TOP_K).astype(jnp.int32)
    blocks = normed.reshape(N_EP, TOK_EP, D)

    def fill(target_rows, block):
        return jnp.zeros((EXPERTS * CAP, D), jnp.bfloat16).at[target_rows].set(block[source])
    buffers = jax.vmap(fill)(targets, blocks)
    per_expert = buffers.reshape(N_EP, EXPERTS, CAP, D).transpose(1, 0, 2, 3).reshape(EXPERTS, N_EP * CAP, D)
    gates = gate_weight.reshape(EXPERTS, 2, D, DE // 2)
    ups = up_weight.reshape(EXPERTS, 2, D, DE // 2)
    downs = down_weight.reshape(EXPERTS, 2, DE // 2, D)
    results = lax.map(expert_rows, (per_expert, gates, ups, downs))
    by_source = results.reshape(EXPERTS, N_EP, CAP, D).transpose(1, 0, 2, 3).reshape(N_EP, EXPERTS * CAP, D)

    def pick(out_rows, target_rows):
        return out_rows[target_rows]
    picked = jax.vmap(pick)(by_source, targets).reshape(TOKENS, TOP_K, D)
    routed = lax.optimization_barrier(jnp.sum(picked * route_weight[:, :, None], axis=1))
    factor_out = lax.rsqrt(lax.optimization_barrier(jnp.mean(routed * routed, axis=1, keepdims=True)) + norm_eps)
    return (routed * factor_out * gain_out).astype(jnp.bfloat16)
```

```python
import functools

import jax
import jax.numpy as jnp
from jax import lax
from jax.experimental import pallas as pl
from jax.experimental.pallas import tpu as pltpu
from jax.sharding import PartitionSpec as P

norm_eps = 1e-06


def plain(
    tokens, gain_in, gain_out, expert_ids, route_weight, gate_weight, up_weight, down_weight
):
    tok_rows, half_width = tokens.shape
    full_width = 2 * half_width
    expert_count = lax.axis_size("ep") // 2
    picks = expert_ids.shape[1]
    capacity = tok_rows * picks * 3 // (2 * expert_count)
    own_cols = lax.axis_index("tp") * half_width
    own_float = tokens.astype(jnp.float32)
    squares = lax.psum(jnp.sum(own_float * own_float, axis=1), "tp")
    factor = lax.rsqrt(squares / full_width + norm_eps)[:, None]
    own_gain = lax.dynamic_slice_in_dim(gain_in, own_cols, half_width)
    normed = (own_float * factor * own_gain).astype(jnp.bfloat16)
    sent_width = normed.shape[1]
    flat_ids = expert_ids.reshape(-1)
    onehot = (flat_ids[:, None] == jnp.arange(expert_count, dtype=jnp.int32)[None, :]).astype(
        jnp.int32
    )
    before = jnp.cumsum(onehot, axis=0) - onehot
    targets = flat_ids * capacity + jnp.sum(before * onehot, axis=1)
    per_token = targets.reshape(tok_rows, picks)
    slot_rows = jnp.arange(expert_count * capacity, dtype=jnp.int32)[:, None]
    placing = jnp.zeros((expert_count * capacity, tok_rows), jnp.bfloat16)
    for which in range(picks):
        placing = placing + (slot_rows == per_token[None, :, which]).astype(jnp.bfloat16)
    packed = jnp.dot(placing, normed, preferred_element_type=jnp.float32).astype(jnp.bfloat16)
    stacked = packed.reshape(expert_count, 1, capacity, sent_width)
    outgoing = jnp.broadcast_to(stacked, (expert_count, 2, capacity, sent_width)).reshape(
        2 * expert_count, capacity, sent_width
    )
    arrived = lax.all_to_all(outgoing, "ep", split_axis=0, concat_axis=0, tiled=True)
    arrived = lax.all_gather(arrived, "tp", axis=2, tiled=True)
    sources = arrived.shape[0]
    gathered = arrived.reshape(sources * capacity, full_width)
    gate_pre = jnp.dot(gathered, gate_weight[0], preferred_element_type=jnp.float32)
    up_pre = jnp.dot(gathered, up_weight[0], preferred_element_type=jnp.float32)
    hidden = (jax.nn.silu(gate_pre) * up_pre).astype(jnp.bfloat16)
    partial_value = jnp.dot(hidden, down_weight[0], preferred_element_type=jnp.float32).astype(
        jnp.bfloat16
    )
    partial_value = partial_value.reshape(sources, capacity, full_width)
    half_sum = lax.psum_scatter(partial_value, "tp", scatter_dimension=2, tiled=True).astype(
        jnp.float32
    )
    returned = lax.all_to_all(
        half_sum.astype(jnp.bfloat16), "ep", split_axis=0, concat_axis=0, tiled=True
    )
    merged = jnp.sum(
        returned.reshape(expert_count, 2, capacity, half_width).astype(jnp.float32), axis=1
    )
    merged = merged.reshape(expert_count * capacity, half_width)
    picked = jnp.take(merged, targets, axis=0).reshape(tok_rows, picks, half_width)
    routed = jnp.sum(picked * route_weight[:, :, None], axis=1)
    squares_out = lax.psum(jnp.sum(routed * routed, axis=1), "tp")
    factor_out = lax.rsqrt(squares_out / full_width + norm_eps)[:, None]
    own_gain_out = lax.dynamic_slice_in_dim(gain_out, own_cols, half_width)
    return (routed * factor_out * own_gain_out).astype(jnp.bfloat16)


MESH = pl.DeviceIdType.MESH


def fused(
    experts,
    cap,
    tok_ref,
    gain_in_ref,
    gain_out_ref,
    ids_ref,
    route_ref,
    gate_hbm,
    up_hbm,
    down_hbm,
    out_ref,
    packed,
    rows,
    parts,
    peer_parts,
    kept,
    crossing,
    crossed,
    leaving,
    home,
    gate_up,
    down,
    sums,
    peer_sums,
    total,
    w_sem,
    sq_send,
    sq_recv,
    line_send,
    line_recv,
    core_send,
    core_recv,
    pair_send,
    pair_recv,
    relay_send,
    relay_recv,
    part_send,
    part_recv,
    cross_send,
    cross_recv,
    home_send,
    home_recv,
):
    tok_rows, width = tok_ref.shape
    hidden_width = down.shape[0]
    place = lax.axis_index("ep")
    core = lax.axis_index("tp")
    half = place % 2
    mine = place // 2
    partner = place + 1 - 2 * half
    other = 1 - core
    own_cols = pl.ds(pl.multiple_of(core * width, 128), width)
    other_cols = pl.ds(pl.multiple_of(other * width, 128), width)

    def on_line(step):
        return 2 * ((mine + step) % experts) + half

    loads = [
        pltpu.make_async_copy(gate_hbm.at[0], gate_up.at[:, pl.ds(0, hidden_width)], w_sem.at[0]),
        pltpu.make_async_copy(
            up_hbm.at[0], gate_up.at[:, pl.ds(hidden_width, hidden_width)], w_sem.at[1]
        ),
        pltpu.make_async_copy(down_hbm.at[0], down, w_sem.at[2]),
    ]
    barrier = pltpu.get_barrier_semaphore()
    pl.semaphore_signal(barrier, inc=1, device_id={"tp": other}, device_id_type=MESH)
    pl.semaphore_signal(barrier, inc=1, device_id={"ep": partner}, device_id_type=MESH)
    for step in range(1, experts):
        pl.semaphore_signal(barrier, inc=1, device_id={"ep": on_line(step)}, device_id_type=MESH)
    for load in loads:
        load.start()

    def remote(source, target, send, recv, device):
        return pltpu.make_async_remote_copy(
            src_ref=source,
            dst_ref=target,
            send_sem=send,
            recv_sem=recv,
            device_id=device,
            device_id_type=MESH,
        )

    def sum_copy(which):
        return remote(
            sums.at[which], peer_sums.at[which], sq_send.at[which], sq_recv.at[which], {"tp": other}
        )

    def line_copy(step):
        back = experts - step
        return remote(
            packed.at[step],
            rows.at[back, 0, :, own_cols],
            line_send.at[back],
            line_recv.at[back],
            {"ep": on_line(step)},
        )

    def core_copy(d):
        view = rows.at[d, 0, :, own_cols]
        return remote(view, view, core_send.at[d], core_recv.at[d], {"tp": other})

    def core_arrival(d):
        view = rows.at[d, 0, :, other_cols]
        return remote(view, view, core_send.at[d], core_recv.at[d], {"tp": other})

    def pair_copy(d):
        return remote(
            rows.at[d, 0, :, own_cols],
            rows.at[d, 1, :, own_cols],
            pair_send.at[d],
            pair_recv.at[d],
            {"ep": partner},
        )

    def relay_copy(d):
        view = rows.at[d, 1, :, own_cols]
        return remote(view, view, relay_send.at[d], relay_recv.at[d], {"tp": other})

    def relay_arrival(d):
        view = rows.at[d, 1, :, other_cols]
        return remote(view, view, relay_send.at[d], relay_recv.at[d], {"tp": other})

    def part_copy(d):
        return remote(
            parts.at[d, :, :, other_cols],
            peer_parts.at[d],
            part_send.at[d],
            part_recv.at[d],
            {"tp": other},
        )

    def cross_copy(d):
        return remote(
            crossing.at[d], crossed.at[d], cross_send.at[d], cross_recv.at[d], {"ep": partner}
        )

    def home_copy(d):
        back = experts - d
        return remote(
            leaving.at[d], home.at[back], home_send.at[back], home_recv.at[back], {"ep": on_line(d)}
        )

    own_float = tok_ref[...].astype(jnp.float32)
    sums[0] = jnp.broadcast_to(
        jnp.sum(own_float * own_float, axis=1, keepdims=True), (tok_rows, 128)
    )
    pl.semaphore_wait(barrier, experts + 1)
    sum_copy(0).start()

    lead = max(8, experts)
    names = lax.broadcasted_iota(jnp.int32, (lead, tok_rows), 0)
    first = names == ids_ref[0:1, :]
    second = names == ids_ref[1:2, :]
    either = (first.astype(jnp.float32) + second.astype(jnp.float32)).astype(jnp.bfloat16)
    earlier = (
        lax.broadcasted_iota(jnp.int32, (tok_rows, tok_rows), 0)
        < lax.broadcasted_iota(jnp.int32, (tok_rows, tok_rows), 1)
    ).astype(jnp.float32).astype(jnp.bfloat16)
    before = jnp.dot(either, earlier, preferred_element_type=jnp.float32)
    slot_one = jnp.sum(jnp.where(first, before, 0.0), axis=0, keepdims=True).astype(jnp.int32)
    slot_two = jnp.sum(jnp.where(second, before, 0.0), axis=0, keepdims=True).astype(jnp.int32)
    target_one = ids_ref[0:1, :] * cap + slot_one
    target_two = ids_ref[1:2, :] * cap + slot_two
    slot_rows = lax.broadcasted_iota(jnp.int32, (cap, tok_rows), 0)

    def hits(step):
        base = ((mine + step) % experts) * cap
        return slot_rows + base == target_one, slot_rows + base == target_two

    sum_copy(0).wait_recv()
    squares = sums[0] + peer_sums[0]
    factor = lax.rsqrt(squares[:, 0:1] / (2 * width) + norm_eps)
    normed = (own_float * factor * gain_in_ref[...]).astype(jnp.bfloat16)

    def pack(step):
        one, two = hits(step)
        placing = (one.astype(jnp.float32) + two.astype(jnp.float32)).astype(jnp.bfloat16)
        return jnp.dot(placing, normed, preferred_element_type=jnp.float32).astype(jnp.bfloat16)

    rows[0, 0, :, own_cols] = pack(0)
    pair_copy(0).start()
    core_copy(0).start()
    for step in range(experts - 1, 0, -1):
        packed[step] = pack(step)
        line_copy(step).start()

    def relay_line(d):
        line_copy(experts - d).wait_recv()
        pair_copy(d).start()
        core_copy(d).start()

    def relay_pair(d):
        pair_copy(d).wait_recv()
        relay_copy(d).start()

    def compute(d):
        core_arrival(d).wait_recv()
        relay_arrival(d).wait_recv()
        block = rows[d].reshape(2 * cap, 2 * width)
        pre = jnp.dot(block, gate_up[...], preferred_element_type=jnp.float32)
        gate_pre = pre[:, :hidden_width]
        hidden = (gate_pre / (1.0 + jnp.exp(-gate_pre)) * pre[:, hidden_width:]).astype(
            jnp.bfloat16
        )
        partial = jnp.dot(hidden, down[...], preferred_element_type=jnp.float32)
        parts[d] = partial.astype(jnp.bfloat16).reshape(2, cap, 2 * width)
        part_copy(d).start()

    def cross(d):
        part_copy(d).wait_recv()
        crossing[d] = (
            parts[d, 1, :, own_cols].astype(jnp.float32) + peer_parts[d, 1].astype(jnp.float32)
        ).astype(jnp.bfloat16)
        cross_copy(d).start()
        kept[d] = parts[d, 0, :, own_cols].astype(jnp.float32) + peer_parts[d, 0].astype(
            jnp.float32
        )

    def send_home(d):
        cross_copy(d).wait_recv()
        return (kept[d] + crossed[d].astype(jnp.float32)).astype(jnp.bfloat16)

    relay_pair(0)
    for load in loads:
        load.wait()

    def step_of(d, carry):
        @pl.when(d + 1 < experts)
        def _():
            relay_line(d + 1)

        compute(d)

        @pl.when(d + 1 < experts)
        def _():
            relay_pair(d + 1)

        cross(d)

        @pl.when(d == 1)
        def _():
            home[0] = send_home(0)

        @pl.when(d > 1)
        def _():
            leaving[d - 1] = send_home(d - 1)
            home_copy(d - 1).start()

        return carry

    lax.fori_loop(0, experts, step_of, 0)
    leaving[experts - 1] = send_home(experts - 1)
    home_copy(experts - 1).start()

    def combine(step):
        one, two = hits(step)
        mix = jnp.where(one, route_ref[0:1, :], 0.0) + jnp.where(two, route_ref[1:2, :], 0.0)
        high = mix.astype(jnp.bfloat16)
        low = (mix - high.astype(jnp.float32)).astype(jnp.bfloat16)
        dims = (((0,), (0,)), ((), ()))
        return lax.dot_general(
            high, home[step], dims, preferred_element_type=jnp.float32
        ) + lax.dot_general(low, home[step], dims, preferred_element_type=jnp.float32)

    total[...] = combine(0)
    for step in range(experts - 1, 0, -1):
        home_copy(experts - step).wait_recv()
        total[...] += combine(step)
    routed = total[...]
    sums[1] = jnp.broadcast_to(jnp.sum(routed * routed, axis=1, keepdims=True), (tok_rows, 128))
    sum_copy(1).start()
    sum_copy(1).wait_recv()
    squares_out = sums[1] + peer_sums[1]
    factor_out = lax.rsqrt(squares_out[:, 0:1] / (2 * width) + norm_eps)
    out_ref[...] = (total[...] * factor_out * gain_out_ref[...]).astype(jnp.bfloat16)

    sum_copy(0).wait_send()
    sum_copy(1).wait_send()

    def drain(d, carry):
        core_copy(d).wait_send()
        pair_copy(d).wait_send()
        relay_copy(d).wait_send()
        part_copy(d).wait_send()
        cross_copy(d).wait_send()

        @pl.when(d > 0)
        def _():
            line_copy(d).wait_send()
            home_copy(d).wait_send()

        return carry

    lax.fori_loop(0, experts, drain, 0)


def layer(
    tokens, gain_in, gain_out, expert_ids, route_weight, gate_weight, up_weight, down_weight
):
    tok_rows, width = tokens.shape
    experts = lax.axis_size("ep") // 2
    picks = expert_ids.shape[1]
    cap = tok_rows * picks * 3 // (2 * experts)
    hidden_width = gate_weight.shape[2]
    if picks != 2 or experts < 2 or cap % 16 or width % 128 or hidden_width % 128:
        return plain(
            tokens, gain_in, gain_out, expert_ids, route_weight, gate_weight, up_weight, down_weight
        )
    own = lax.axis_index("tp") * width
    own_gain_in = lax.dynamic_slice_in_dim(gain_in, own, width)[None, :]
    own_gain_out = lax.dynamic_slice_in_dim(gain_out, own, width)[None, :]
    vmem = pl.BlockSpec(memory_space=pltpu.VMEM)
    hbm = pl.BlockSpec(memory_space=pl.ANY)
    bf16, f32 = jnp.bfloat16, jnp.float32
    lines = [pltpu.SemaphoreType.DMA((experts,))] * 14
    return pl.pallas_call(
        functools.partial(fused, experts, cap),
        out_shape=jax.ShapeDtypeStruct((tok_rows, width), bf16),
        in_specs=[vmem] * 5 + [hbm] * 3,
        out_specs=vmem,
        scratch_shapes=[
            pltpu.VMEM((experts, cap, width), bf16),
            pltpu.VMEM((experts, 2, cap, 2 * width), bf16),
            pltpu.VMEM((experts, 2, cap, 2 * width), bf16),
            pltpu.VMEM((experts, 2, cap, width), bf16),
            pltpu.VMEM((experts, cap, width), f32),
            pltpu.VMEM((experts, cap, width), bf16),
            pltpu.VMEM((experts, cap, width), bf16),
            pltpu.VMEM((experts, cap, width), bf16),
            pltpu.VMEM((experts, cap, width), bf16),
            pltpu.VMEM((2 * width, 2 * hidden_width), bf16),
            pltpu.VMEM((hidden_width, 2 * width), bf16),
            pltpu.VMEM((2, tok_rows, 128), f32),
            pltpu.VMEM((2, tok_rows, 128), f32),
            pltpu.VMEM((tok_rows, width), f32),
            pltpu.SemaphoreType.DMA((3,)),
            pltpu.SemaphoreType.DMA((2,)),
            pltpu.SemaphoreType.DMA((2,)),
        ]
        + lines,
        compiler_params=pltpu.CompilerParams(
            collective_id=0, has_side_effects=True, vmem_limit_bytes=60 * 1024 * 1024
        ),
    )(
        tokens,
        own_gain_in,
        own_gain_out,
        expert_ids.T,
        route_weight.T,
        gate_weight,
        up_weight,
        down_weight,
    )


def solution(mesh):
    in_specs = (
        P(("grp", "ep"), "tp"),
        P(),
        P(),
        P(("grp", "ep"), None),
        P(("grp", "ep"), None),
        P("ep", None, "tp"),
        P("ep", None, "tp"),
        P("ep", "tp", None),
    )
    out_specs = P(("grp", "ep"), "tp")
    return jax.shard_map(layer, mesh=mesh, in_specs=in_specs, out_specs=out_specs, check_vma=False)
```

```python
import functools

import jax
import jax.numpy as jnp
from jax import lax
from jax.experimental import pallas as pl
from jax.experimental.pallas import tpu as pltpu
from jax.sharding import PartitionSpec as P

norm_eps = 1e-06


def plain(
    tokens, gain_in, gain_out, expert_ids, route_weight, gate_weight, up_weight, down_weight
):
    tok_rows, half_width = tokens.shape
    full_width = 2 * half_width
    expert_count = lax.axis_size("ep") // 2
    picks = expert_ids.shape[1]
    capacity = tok_rows * picks * 3 // (2 * expert_count)
    own_cols = lax.axis_index("tp") * half_width
    own_float = tokens.astype(jnp.float32)
    squares = lax.psum(jnp.sum(own_float * own_float, axis=1), "tp")
    factor = lax.rsqrt(squares / full_width + norm_eps)[:, None]
    own_gain = lax.dynamic_slice_in_dim(gain_in, own_cols, half_width)
    normed = (own_float * factor * own_gain).astype(jnp.bfloat16)
    sent_width = normed.shape[1]
    flat_ids = expert_ids.reshape(-1)
    onehot = (flat_ids[:, None] == jnp.arange(expert_count, dtype=jnp.int32)[None, :]).astype(
        jnp.int32
    )
    before = jnp.cumsum(onehot, axis=0) - onehot
    targets = flat_ids * capacity + jnp.sum(before * onehot, axis=1)
    per_token = targets.reshape(tok_rows, picks)
    slot_rows = jnp.arange(expert_count * capacity, dtype=jnp.int32)[:, None]
    placing = jnp.zeros((expert_count * capacity, tok_rows), jnp.bfloat16)
    for which in range(picks):
        placing = placing + (slot_rows == per_token[None, :, which]).astype(jnp.bfloat16)
    packed = jnp.dot(placing, normed, preferred_element_type=jnp.float32).astype(jnp.bfloat16)
    stacked = packed.reshape(expert_count, 1, capacity, sent_width)
    outgoing = jnp.broadcast_to(stacked, (expert_count, 2, capacity, sent_width)).reshape(
        2 * expert_count, capacity, sent_width
    )
    arrived = lax.all_to_all(outgoing, "ep", split_axis=0, concat_axis=0, tiled=True)
    arrived = lax.all_gather(arrived, "tp", axis=2, tiled=True)
    sources = arrived.shape[0]
    gathered = arrived.reshape(sources * capacity, full_width)
    gate_pre = jnp.dot(gathered, gate_weight[0], preferred_element_type=jnp.float32)
    up_pre = jnp.dot(gathered, up_weight[0], preferred_element_type=jnp.float32)
    hidden = (jax.nn.silu(gate_pre) * up_pre).astype(jnp.bfloat16)
    partial_value = jnp.dot(hidden, down_weight[0], preferred_element_type=jnp.float32).astype(
        jnp.bfloat16
    )
    partial_value = partial_value.reshape(sources, capacity, full_width)
    half_sum = lax.psum_scatter(partial_value, "tp", scatter_dimension=2, tiled=True).astype(
        jnp.float32
    )
    returned = lax.all_to_all(
        half_sum.astype(jnp.bfloat16), "ep", split_axis=0, concat_axis=0, tiled=True
    )
    merged = jnp.sum(
        returned.reshape(expert_count, 2, capacity, half_width).astype(jnp.float32), axis=1
    )
    merged = merged.reshape(expert_count * capacity, half_width)
    picked = jnp.take(merged, targets, axis=0).reshape(tok_rows, picks, half_width)
    routed = jnp.sum(picked * route_weight[:, :, None], axis=1)
    squares_out = lax.psum(jnp.sum(routed * routed, axis=1), "tp")
    factor_out = lax.rsqrt(squares_out / full_width + norm_eps)[:, None]
    own_gain_out = lax.dynamic_slice_in_dim(gain_out, own_cols, half_width)
    return (routed * factor_out * own_gain_out).astype(jnp.bfloat16)


MESH = pl.DeviceIdType.MESH


def fused(
    experts,
    cap,
    tok_ref,
    gain_in_ref,
    gain_out_ref,
    ids_ref,
    route_ref,
    gate_hbm,
    up_hbm,
    down_hbm,
    out_ref,
    packed,
    rows,
    parts,
    peer_parts,
    kept,
    crossing,
    crossed,
    leaving,
    home,
    gate_up,
    down,
    sums,
    peer_sums,
    total,
    w_sem,
    sq_send,
    sq_recv,
    line_send,
    line_recv,
    core_send,
    core_recv,
    pair_send,
    pair_recv,
    relay_send,
    relay_recv,
    part_send,
    part_recv,
    cross_send,
    cross_recv,
    home_send,
    home_recv,
):
    tok_rows, width = tok_ref.shape
    hidden_width = down.shape[0]
    place = lax.axis_index("ep")
    core = lax.axis_index("tp")
    half = place % 2
    mine = place // 2
    partner = place + 1 - 2 * half
    other = 1 - core
    own_cols = pl.ds(pl.multiple_of(core * width, 128), width)
    other_cols = pl.ds(pl.multiple_of(other * width, 128), width)

    way = 1 - 2 * (2 * mine // experts)
    near = mine * (1 + way) // 2 + (experts - 1 - mine) * (1 - way) // 2

    def nearest(turn):
        both = jnp.where(turn % 2 == 1, -way, way) * ((turn + 1) // 2)
        return (jnp.where(turn <= 2 * near, both, way * (turn - near)) + experts) % experts

    def on_line(step):
        return 2 * ((mine + step) % experts) + half

    loads = [
        pltpu.make_async_copy(gate_hbm.at[0], gate_up.at[:, pl.ds(0, hidden_width)], w_sem.at[0]),
        pltpu.make_async_copy(
            up_hbm.at[0], gate_up.at[:, pl.ds(hidden_width, hidden_width)], w_sem.at[1]
        ),
        pltpu.make_async_copy(down_hbm.at[0], down, w_sem.at[2]),
    ]
    barrier = pltpu.get_barrier_semaphore()
    pl.semaphore_signal(barrier, inc=1, device_id={"tp": other}, device_id_type=MESH)
    pl.semaphore_signal(barrier, inc=1, device_id={"ep": partner}, device_id_type=MESH)
    for step in range(1, experts):
        pl.semaphore_signal(barrier, inc=1, device_id={"ep": on_line(step)}, device_id_type=MESH)
    for load in loads:
        load.start()

    def remote(source, target, send, recv, device):
        return pltpu.make_async_remote_copy(
            src_ref=source,
            dst_ref=target,
            send_sem=send,
            recv_sem=recv,
            device_id=device,
            device_id_type=MESH,
        )

    def sum_copy(which):
        return remote(
            sums.at[which], peer_sums.at[which], sq_send.at[which], sq_recv.at[which], {"tp": other}
        )

    def line_copy(step):
        back = experts - step
        return remote(
            packed.at[step],
            rows.at[back, 0, :, own_cols],
            line_send.at[back],
            line_recv.at[back],
            {"ep": on_line(step)},
        )

    def core_copy(d):
        view = rows.at[d, 0, :, own_cols]
        return remote(view, view, core_send.at[d], core_recv.at[d], {"tp": other})

    def core_arrival(d):
        view = rows.at[d, 0, :, other_cols]
        return remote(view, view, core_send.at[d], core_recv.at[d], {"tp": other})

    def pair_copy(d):
        return remote(
            rows.at[d, 0, :, own_cols],
            rows.at[d, 1, :, own_cols],
            pair_send.at[d],
            pair_recv.at[d],
            {"ep": partner},
        )

    def relay_copy(d):
        view = rows.at[d, 1, :, own_cols]
        return remote(view, view, relay_send.at[d], relay_recv.at[d], {"tp": other})

    def relay_arrival(d):
        view = rows.at[d, 1, :, other_cols]
        return remote(view, view, relay_send.at[d], relay_recv.at[d], {"tp": other})

    def part_copy(d):
        return remote(
            parts.at[d, :, :, other_cols],
            peer_parts.at[d],
            part_send.at[d],
            part_recv.at[d],
            {"tp": other},
        )

    def cross_copy(d):
        return remote(
            crossing.at[d], crossed.at[d], cross_send.at[d], cross_recv.at[d], {"ep": partner}
        )

    def home_copy(d):
        back = experts - d
        return remote(
            leaving.at[d], home.at[back], home_send.at[back], home_recv.at[back], {"ep": on_line(d)}
        )

    own_float = tok_ref[...].astype(jnp.float32)
    sums[0] = jnp.broadcast_to(
        jnp.sum(own_float * own_float, axis=1, keepdims=True), (tok_rows, 128)
    )
    pl.semaphore_wait(barrier, experts + 1)
    sum_copy(0).start()

    lead = max(8, experts)
    names = lax.broadcasted_iota(jnp.int32, (lead, tok_rows), 0)
    first = names == ids_ref[0:1, :]
    second = names == ids_ref[1:2, :]
    either = (first.astype(jnp.float32) + second.astype(jnp.float32)).astype(jnp.bfloat16)
    earlier = (
        lax.broadcasted_iota(jnp.int32, (tok_rows, tok_rows), 0)
        < lax.broadcasted_iota(jnp.int32, (tok_rows, tok_rows), 1)
    ).astype(jnp.float32).astype(jnp.bfloat16)
    before = jnp.dot(either, earlier, preferred_element_type=jnp.float32)
    slot_one = jnp.sum(jnp.where(first, before, 0.0), axis=0, keepdims=True).astype(jnp.int32)
    slot_two = jnp.sum(jnp.where(second, before, 0.0), axis=0, keepdims=True).astype(jnp.int32)
    target_one = ids_ref[0:1, :] * cap + slot_one
    target_two = ids_ref[1:2, :] * cap + slot_two
    slot_rows = lax.broadcasted_iota(jnp.int32, (cap, tok_rows), 0)

    def hits(step):
        base = ((mine + step) % experts) * cap
        return slot_rows + base == target_one, slot_rows + base == target_two

    sum_copy(0).wait_recv()
    squares = sums[0] + peer_sums[0]
    factor = lax.rsqrt(squares[:, 0:1] / (2 * width) + norm_eps)
    normed = (own_float * factor * gain_in_ref[:, own_cols]).astype(jnp.bfloat16)

    def pack(step):
        one, two = hits(step)
        placing = (one.astype(jnp.float32) + two.astype(jnp.float32)).astype(jnp.bfloat16)
        return jnp.dot(placing, normed, preferred_element_type=jnp.float32).astype(jnp.bfloat16)

    rows[0, 0, :, own_cols] = pack(0)
    pair_copy(0).start()
    core_copy(0).start()
    for turn in range(1, experts):
        step = nearest(turn)
        packed[step] = pack(step)
        line_copy(step).start()

    def relay_line(d):
        line_copy(experts - d).wait_recv()
        pair_copy(d).start()
        core_copy(d).start()

    def relay_pair(d):
        pair_copy(d).wait_recv()
        relay_copy(d).start()

    def compute(d):
        core_arrival(d).wait_recv()
        relay_arrival(d).wait_recv()
        block = rows[d].reshape(2 * cap, 2 * width)
        pre = jnp.dot(block, gate_up[...], preferred_element_type=jnp.float32)
        gate_pre = pre[:, :hidden_width]
        hidden = (gate_pre / (1.0 + jnp.exp(-gate_pre)) * pre[:, hidden_width:]).astype(
            jnp.bfloat16
        )
        partial = jnp.dot(hidden, down[...], preferred_element_type=jnp.float32)
        parts[d] = partial.astype(jnp.bfloat16).reshape(2, cap, 2 * width)
        part_copy(d).start()

    def cross(d):
        part_copy(d).wait_recv()
        crossing[d] = (
            parts[d, 1, :, own_cols].astype(jnp.float32) + peer_parts[d, 1].astype(jnp.float32)
        ).astype(jnp.bfloat16)
        cross_copy(d).start()
        kept[d] = parts[d, 0, :, own_cols].astype(jnp.float32) + peer_parts[d, 0].astype(
            jnp.float32
        )

    def send_home(d):
        cross_copy(d).wait_recv()
        return (kept[d] + crossed[d].astype(jnp.float32)).astype(jnp.bfloat16)

    relay_line(nearest(1))
    relay_pair(0)
    for load in loads:
        load.wait()

    def step_of(turn, carry):
        d = nearest(turn)
        compute(d)

        @pl.when((turn > 0) & (turn + 1 < experts))
        def _():
            relay_line(nearest(turn + 1))

        cross(d)

        @pl.when(turn == 1)
        def _():
            home[0] = send_home(0)

        @pl.when(turn > 1)
        def _():
            last = nearest(turn - 1)
            leaving[last] = send_home(last)
            home_copy(last).start()

        @pl.when(turn + 1 < experts)
        def _():
            relay_pair(nearest(turn + 1))

        return carry

    lax.fori_loop(0, experts, step_of, 0)
    final = nearest(experts - 1)
    leaving[final] = send_home(final)
    home_copy(final).start()

    def combine(step):
        one, two = hits(step)
        mix = jnp.where(one, route_ref[0:1, :], 0.0) + jnp.where(two, route_ref[1:2, :], 0.0)
        high = mix.astype(jnp.bfloat16)
        low = (mix - high.astype(jnp.float32)).astype(jnp.bfloat16)
        dims = (((0,), (0,)), ((), ()))
        return lax.dot_general(
            high, home[step], dims, preferred_element_type=jnp.float32
        ) + lax.dot_general(low, home[step], dims, preferred_element_type=jnp.float32)

    total[...] = combine(0)
    for turn in range(1, experts):
        step = nearest(turn)
        home_copy(experts - step).wait_recv()
        total[...] += combine(step)
    routed = total[...]
    sums[1] = jnp.broadcast_to(jnp.sum(routed * routed, axis=1, keepdims=True), (tok_rows, 128))
    sum_copy(1).start()
    sum_copy(1).wait_recv()
    squares_out = sums[1] + peer_sums[1]
    factor_out = lax.rsqrt(squares_out[:, 0:1] / (2 * width) + norm_eps)
    out_ref[...] = (total[...] * factor_out * gain_out_ref[:, own_cols]).astype(jnp.bfloat16)

    sum_copy(0).wait_send()
    sum_copy(1).wait_send()

    def drain(d, carry):
        core_copy(d).wait_send()
        pair_copy(d).wait_send()
        relay_copy(d).wait_send()
        part_copy(d).wait_send()
        cross_copy(d).wait_send()

        @pl.when(d > 0)
        def _():
            line_copy(d).wait_send()
            home_copy(d).wait_send()

        return carry

    lax.fori_loop(0, experts, drain, 0)


def layer(
    tokens, gain_in, gain_out, expert_ids, route_weight, gate_weight, up_weight, down_weight
):
    tok_rows, width = tokens.shape
    experts = lax.axis_size("ep") // 2
    picks = expert_ids.shape[1]
    cap = tok_rows * picks * 3 // (2 * experts)
    hidden_width = gate_weight.shape[2]
    if picks != 2 or experts < 2 or cap % 16 or width % 128 or hidden_width % 128:
        return plain(
            tokens, gain_in, gain_out, expert_ids, route_weight, gate_weight, up_weight, down_weight
        )
    vmem = pl.BlockSpec(memory_space=pltpu.VMEM)
    hbm = pl.BlockSpec(memory_space=pl.ANY)
    bf16, f32 = jnp.bfloat16, jnp.float32
    lines = [pltpu.SemaphoreType.DMA((experts,))] * 14
    return pl.pallas_call(
        functools.partial(fused, experts, cap),
        out_shape=jax.ShapeDtypeStruct((tok_rows, width), bf16),
        in_specs=[vmem] * 5 + [hbm] * 3,
        out_specs=vmem,
        scratch_shapes=[
            pltpu.VMEM((experts, cap, width), bf16),
            pltpu.VMEM((experts, 2, cap, 2 * width), bf16),
            pltpu.VMEM((experts, 2, cap, 2 * width), bf16),
            pltpu.VMEM((experts, 2, cap, width), bf16),
            pltpu.VMEM((experts, cap, width), f32),
            pltpu.VMEM((experts, cap, width), bf16),
            pltpu.VMEM((experts, cap, width), bf16),
            pltpu.VMEM((experts, cap, width), bf16),
            pltpu.VMEM((experts, cap, width), bf16),
            pltpu.VMEM((2 * width, 2 * hidden_width), bf16),
            pltpu.VMEM((hidden_width, 2 * width), bf16),
            pltpu.VMEM((2, tok_rows, 128), f32),
            pltpu.VMEM((2, tok_rows, 128), f32),
            pltpu.VMEM((tok_rows, width), f32),
            pltpu.SemaphoreType.DMA((3,)),
            pltpu.SemaphoreType.DMA((2,)),
            pltpu.SemaphoreType.DMA((2,)),
        ]
        + lines,
        compiler_params=pltpu.CompilerParams(
            collective_id=0, has_side_effects=True, vmem_limit_bytes=60 * 1024 * 1024
        ),
    )(
        tokens,
        gain_in[None, :],
        gain_out[None, :],
        expert_ids.T,
        route_weight.T,
        gate_weight,
        up_weight,
        down_weight,
    )


def solution(mesh):
    in_specs = (
        P(("grp", "ep"), "tp"),
        P(),
        P(),
        P(("grp", "ep"), None),
        P(("grp", "ep"), None),
        P("ep", None, "tp"),
        P("ep", None, "tp"),
        P("ep", "tp", None),
    )
    out_specs = P(("grp", "ep"), "tp")
    return jax.shard_map(layer, mesh=mesh, in_specs=in_specs, out_specs=out_specs, check_vma=False)
```

```python
import functools

import jax
import jax.numpy as jnp
from jax import lax
from jax.experimental import pallas as pl
from jax.experimental.pallas import tpu as pltpu
from jax.sharding import PartitionSpec as P

norm_eps = 1e-06


def plain(
    tokens, gain_in, gain_out, expert_ids, route_weight, gate_weight, up_weight, down_weight
):
    tok_rows, half_width = tokens.shape
    full_width = 2 * half_width
    expert_count = lax.axis_size("ep") // 2
    picks = expert_ids.shape[1]
    capacity = tok_rows * picks * 3 // (2 * expert_count)
    own_cols = lax.axis_index("tp") * half_width
    own_float = tokens.astype(jnp.float32)
    squares = lax.psum(jnp.sum(own_float * own_float, axis=1), "tp")
    factor = lax.rsqrt(squares / full_width + norm_eps)[:, None]
    own_gain = lax.dynamic_slice_in_dim(gain_in, own_cols, half_width)
    normed = (own_float * factor * own_gain).astype(jnp.bfloat16)
    sent_width = normed.shape[1]
    flat_ids = expert_ids.reshape(-1)
    onehot = (flat_ids[:, None] == jnp.arange(expert_count, dtype=jnp.int32)[None, :]).astype(
        jnp.int32
    )
    before = jnp.cumsum(onehot, axis=0) - onehot
    targets = flat_ids * capacity + jnp.sum(before * onehot, axis=1)
    per_token = targets.reshape(tok_rows, picks)
    slot_rows = jnp.arange(expert_count * capacity, dtype=jnp.int32)[:, None]
    placing = jnp.zeros((expert_count * capacity, tok_rows), jnp.bfloat16)
    for which in range(picks):
        placing = placing + (slot_rows == per_token[None, :, which]).astype(jnp.bfloat16)
    packed = jnp.dot(placing, normed, preferred_element_type=jnp.float32).astype(jnp.bfloat16)
    stacked = packed.reshape(expert_count, 1, capacity, sent_width)
    outgoing = jnp.broadcast_to(stacked, (expert_count, 2, capacity, sent_width)).reshape(
        2 * expert_count, capacity, sent_width
    )
    arrived = lax.all_to_all(outgoing, "ep", split_axis=0, concat_axis=0, tiled=True)
    arrived = lax.all_gather(arrived, "tp", axis=2, tiled=True)
    sources = arrived.shape[0]
    gathered = arrived.reshape(sources * capacity, full_width)
    gate_pre = jnp.dot(gathered, gate_weight[0], preferred_element_type=jnp.float32)
    up_pre = jnp.dot(gathered, up_weight[0], preferred_element_type=jnp.float32)
    hidden = (jax.nn.silu(gate_pre) * up_pre).astype(jnp.bfloat16)
    partial_value = jnp.dot(hidden, down_weight[0], preferred_element_type=jnp.float32).astype(
        jnp.bfloat16
    )
    partial_value = partial_value.reshape(sources, capacity, full_width)
    half_sum = lax.psum_scatter(partial_value, "tp", scatter_dimension=2, tiled=True).astype(
        jnp.float32
    )
    returned = lax.all_to_all(
        half_sum.astype(jnp.bfloat16), "ep", split_axis=0, concat_axis=0, tiled=True
    )
    merged = jnp.sum(
        returned.reshape(expert_count, 2, capacity, half_width).astype(jnp.float32), axis=1
    )
    merged = merged.reshape(expert_count * capacity, half_width)
    picked = jnp.take(merged, targets, axis=0).reshape(tok_rows, picks, half_width)
    routed = jnp.sum(picked * route_weight[:, :, None], axis=1)
    squares_out = lax.psum(jnp.sum(routed * routed, axis=1), "tp")
    factor_out = lax.rsqrt(squares_out / full_width + norm_eps)[:, None]
    own_gain_out = lax.dynamic_slice_in_dim(gain_out, own_cols, half_width)
    return (routed * factor_out * own_gain_out).astype(jnp.bfloat16)


MESH = pl.DeviceIdType.MESH
pieces = 2


def fused(
    experts,
    cap,
    tok_ref,
    gain_in_ref,
    gain_out_ref,
    ids_ref,
    route_ref,
    gate_hbm,
    up_hbm,
    down_hbm,
    out_ref,
    packed,
    rows,
    parts,
    peer_parts,
    kept,
    crossing,
    crossed,
    leaving,
    home,
    gate_up,
    down,
    sums,
    peer_sums,
    total,
    w_sem,
    sq_send,
    sq_recv,
    line_send,
    line_recv,
    core_send,
    core_recv,
    pair_send,
    pair_recv,
    relay_send,
    relay_recv,
    part_send,
    part_recv,
    cross_send,
    cross_recv,
    home_send,
    home_recv,
):
    tok_rows, width = tok_ref.shape
    hidden_width = down.shape[0]
    place = lax.axis_index("ep")
    core = lax.axis_index("tp")
    half = place % 2
    mine = place // 2
    partner = place + 1 - 2 * half
    other = 1 - core
    own_cols = pl.ds(pl.multiple_of(core * width, 128), width)
    other_cols = pl.ds(pl.multiple_of(other * width, 128), width)

    piece = width // pieces

    def cut(s):
        return pl.ds(s * piece, piece)

    def of_core(which, s):
        return pl.ds(pl.multiple_of(which * width + s * piece, 128), piece)

    def on_line(step):
        return 2 * ((mine + step) % experts) + half

    loads = [
        pltpu.make_async_copy(gate_hbm.at[0], gate_up.at[:, pl.ds(0, hidden_width)], w_sem.at[0]),
        pltpu.make_async_copy(
            up_hbm.at[0], gate_up.at[:, pl.ds(hidden_width, hidden_width)], w_sem.at[1]
        ),
        pltpu.make_async_copy(down_hbm.at[0], down, w_sem.at[2]),
    ]
    barrier = pltpu.get_barrier_semaphore()
    pl.semaphore_signal(barrier, inc=1, device_id={"tp": other}, device_id_type=MESH)
    pl.semaphore_signal(barrier, inc=1, device_id={"ep": partner}, device_id_type=MESH)
    for step in range(1, experts):
        pl.semaphore_signal(barrier, inc=1, device_id={"ep": on_line(step)}, device_id_type=MESH)
    for load in loads:
        load.start()

    def remote(source, target, send, recv, device):
        return pltpu.make_async_remote_copy(
            src_ref=source,
            dst_ref=target,
            send_sem=send,
            recv_sem=recv,
            device_id=device,
            device_id_type=MESH,
        )

    def sum_copy(which):
        return remote(
            sums.at[which], peer_sums.at[which], sq_send.at[which], sq_recv.at[which], {"tp": other}
        )

    def line_copy(step, s):
        back = experts - step
        return remote(
            packed.at[step, :, cut(s)],
            rows.at[back, 0, :, of_core(core, s)],
            line_send.at[back * pieces + s],
            line_recv.at[back * pieces + s],
            {"ep": on_line(step)},
        )

    def core_copy(d, s, which=core):
        view, sem = rows.at[d, 0, :, of_core(which, s)], d * pieces + s
        return remote(view, view, core_send.at[sem], core_recv.at[sem], {"tp": other})

    def pair_copy(d, s):
        return remote(
            rows.at[d, 0, :, of_core(core, s)],
            rows.at[d, 1, :, of_core(core, s)],
            pair_send.at[d * pieces + s],
            pair_recv.at[d * pieces + s],
            {"ep": partner},
        )

    def relay_copy(d, s, which=core):
        view, sem = rows.at[d, 1, :, of_core(which, s)], d * pieces + s
        return remote(view, view, relay_send.at[sem], relay_recv.at[sem], {"tp": other})

    def part_copy(d):
        return remote(
            parts.at[d, :, :, other_cols],
            peer_parts.at[d],
            part_send.at[d],
            part_recv.at[d],
            {"tp": other},
        )

    def cross_copy(d, s):
        sem = d * pieces + s
        return remote(
            crossing.at[d, :, cut(s)],
            crossed.at[d, :, cut(s)],
            cross_send.at[sem],
            cross_recv.at[sem],
            {"ep": partner},
        )

    def home_copy(d, s):
        back = experts - d
        sem = back * pieces + s
        return remote(
            leaving.at[d, :, cut(s)],
            home.at[back, :, cut(s)],
            home_send.at[sem],
            home_recv.at[sem],
            {"ep": on_line(d)},
        )

    own_float = tok_ref[...].astype(jnp.float32)
    sums[0] = jnp.broadcast_to(
        jnp.sum(own_float * own_float, axis=1, keepdims=True), (tok_rows, 128)
    )
    pl.semaphore_wait(barrier, experts + 1)
    sum_copy(0).start()

    lead = max(8, experts)
    names = lax.broadcasted_iota(jnp.int32, (lead, tok_rows), 0)
    first = names == ids_ref[0:1, :]
    second = names == ids_ref[1:2, :]
    either = (first.astype(jnp.float32) + second.astype(jnp.float32)).astype(jnp.bfloat16)
    earlier = (
        lax.broadcasted_iota(jnp.int32, (tok_rows, tok_rows), 0)
        < lax.broadcasted_iota(jnp.int32, (tok_rows, tok_rows), 1)
    ).astype(jnp.float32).astype(jnp.bfloat16)
    before = jnp.dot(either, earlier, preferred_element_type=jnp.float32)
    slot_one = jnp.sum(jnp.where(first, before, 0.0), axis=0, keepdims=True).astype(jnp.int32)
    slot_two = jnp.sum(jnp.where(second, before, 0.0), axis=0, keepdims=True).astype(jnp.int32)
    target_one = ids_ref[0:1, :] * cap + slot_one
    target_two = ids_ref[1:2, :] * cap + slot_two
    slot_rows = lax.broadcasted_iota(jnp.int32, (cap, tok_rows), 0)

    def hits(step):
        base = ((mine + step) % experts) * cap
        return slot_rows + base == target_one, slot_rows + base == target_two

    sum_copy(0).wait_recv()
    squares = sums[0] + peer_sums[0]
    factor = lax.rsqrt(squares[:, 0:1] / (2 * width) + norm_eps)
    normed = (own_float * factor * gain_in_ref[:, own_cols]).astype(jnp.bfloat16)

    def pack(step):
        one, two = hits(step)
        placing = (one.astype(jnp.float32) + two.astype(jnp.float32)).astype(jnp.bfloat16)
        return jnp.dot(placing, normed, preferred_element_type=jnp.float32).astype(jnp.bfloat16)

    rows[0, 0, :, own_cols] = pack(0)
    for s in range(pieces):
        pair_copy(0, s).start()
        core_copy(0, s).start()
    for step in range(experts - 1, 0, -1):
        packed[step] = pack(step)
        for s in range(pieces):
            line_copy(step, s).start()

    def relay_line(d):
        for s in range(pieces):
            line_copy(experts - d, s).wait_recv()
            pair_copy(d, s).start()
            core_copy(d, s).start()

    def relay_pair(d):
        for s in range(pieces):
            pair_copy(d, s).wait_recv()
            relay_copy(d, s).start()

    def compute(d):
        for s in range(pieces):
            core_copy(d, s, other).wait_recv()
            relay_copy(d, s, other).wait_recv()
        block = rows[d].reshape(2 * cap, 2 * width)
        pre = jnp.dot(block, gate_up[...], preferred_element_type=jnp.float32)
        gate_pre = pre[:, :hidden_width]
        hidden = (gate_pre / (1.0 + jnp.exp(-gate_pre)) * pre[:, hidden_width:]).astype(
            jnp.bfloat16
        )
        partial = jnp.dot(hidden, down[...], preferred_element_type=jnp.float32)
        parts[d] = partial.astype(jnp.bfloat16).reshape(2, cap, 2 * width)
        part_copy(d).start()

    def cross(d):
        part_copy(d).wait_recv()
        for s in range(pieces):
            crossing[d, :, cut(s)] = (
                parts[d, 1, :, of_core(core, s)].astype(jnp.float32)
                + peer_parts[d, 1, :, cut(s)].astype(jnp.float32)
            ).astype(jnp.bfloat16)
            cross_copy(d, s).start()
        kept[d] = parts[d, 0, :, own_cols].astype(jnp.float32) + peer_parts[d, 0].astype(
            jnp.float32
        )

    def meet(d, s):
        cross_copy(d, s).wait_recv()
        return (kept[d, :, cut(s)] + crossed[d, :, cut(s)].astype(jnp.float32)).astype(
            jnp.bfloat16
        )

    def keep_own():
        for s in range(pieces):
            home[0, :, cut(s)] = meet(0, s)

    def send_home(d):
        for s in range(pieces):
            leaving[d, :, cut(s)] = meet(d, s)
            home_copy(d, s).start()

    relay_pair(0)
    for load in loads:
        load.wait()

    def step_of(d, carry):
        @pl.when(d + 1 < experts)
        def _():
            relay_line(d + 1)

        compute(d)

        @pl.when(d + 1 < experts)
        def _():
            relay_pair(d + 1)

        cross(d)

        @pl.when(d == 1)
        def _():
            keep_own()

        @pl.when(d > 1)
        def _():
            send_home(d - 1)

        return carry

    lax.fori_loop(0, experts, step_of, 0)
    send_home(experts - 1)

    def weights_of(step):
        one, two = hits(step)
        mix = jnp.where(one, route_ref[0:1, :], 0.0) + jnp.where(two, route_ref[1:2, :], 0.0)
        high = mix.astype(jnp.bfloat16)
        return high, (mix - high.astype(jnp.float32)).astype(jnp.bfloat16)

    def combine(step, s, high, low):
        dims = (((0,), (0,)), ((), ()))
        values = home[step, :, cut(s)]
        return lax.dot_general(
            high, values, dims, preferred_element_type=jnp.float32
        ) + lax.dot_general(low, values, dims, preferred_element_type=jnp.float32)

    mixes = weights_of(0)
    for s in range(pieces):
        total[:, cut(s)] = combine(0, s, *mixes)
    for step in range(experts - 1, 0, -1):
        mixes = weights_of(step)
        for s in range(pieces):
            home_copy(experts - step, s).wait_recv()
            total[:, cut(s)] += combine(step, s, *mixes)
    routed = total[...]
    sums[1] = jnp.broadcast_to(jnp.sum(routed * routed, axis=1, keepdims=True), (tok_rows, 128))
    sum_copy(1).start()
    sum_copy(1).wait_recv()
    squares_out = sums[1] + peer_sums[1]
    factor_out = lax.rsqrt(squares_out[:, 0:1] / (2 * width) + norm_eps)
    out_ref[...] = (total[...] * factor_out * gain_out_ref[:, own_cols]).astype(jnp.bfloat16)

    sum_copy(0).wait_send()
    sum_copy(1).wait_send()

    def drain(d, carry):
        for s in range(pieces):
            core_copy(d, s).wait_send()
            pair_copy(d, s).wait_send()
            relay_copy(d, s).wait_send()
            cross_copy(d, s).wait_send()
        part_copy(d).wait_send()

        @pl.when(d > 0)
        def _():
            for s in range(pieces):
                line_copy(d, s).wait_send()
                home_copy(d, s).wait_send()

        return carry

    lax.fori_loop(0, experts, drain, 0)


def layer(
    tokens, gain_in, gain_out, expert_ids, route_weight, gate_weight, up_weight, down_weight
):
    tok_rows, width = tokens.shape
    experts = lax.axis_size("ep") // 2
    picks = expert_ids.shape[1]
    cap = tok_rows * picks * 3 // (2 * experts)
    hidden_width = gate_weight.shape[2]
    if picks != 2 or experts < 2 or cap % 16 or width % (128 * pieces) or hidden_width % 128:
        return plain(
            tokens, gain_in, gain_out, expert_ids, route_weight, gate_weight, up_weight, down_weight
        )
    vmem = pl.BlockSpec(memory_space=pltpu.VMEM)
    hbm = pl.BlockSpec(memory_space=pl.ANY)
    bf16, f32 = jnp.bfloat16, jnp.float32
    lines = [pltpu.SemaphoreType.DMA((experts * pieces,))] * 14
    return pl.pallas_call(
        functools.partial(fused, experts, cap),
        out_shape=jax.ShapeDtypeStruct((tok_rows, width), bf16),
        in_specs=[vmem] * 5 + [hbm] * 3,
        out_specs=vmem,
        scratch_shapes=[
            pltpu.VMEM((experts, cap, width), bf16),
            pltpu.VMEM((experts, 2, cap, 2 * width), bf16),
            pltpu.VMEM((experts, 2, cap, 2 * width), bf16),
            pltpu.VMEM((experts, 2, cap, width), bf16),
            pltpu.VMEM((experts, cap, width), f32),
            pltpu.VMEM((experts, cap, width), bf16),
            pltpu.VMEM((experts, cap, width), bf16),
            pltpu.VMEM((experts, cap, width), bf16),
            pltpu.VMEM((experts, cap, width), bf16),
            pltpu.VMEM((2 * width, 2 * hidden_width), bf16),
            pltpu.VMEM((hidden_width, 2 * width), bf16),
            pltpu.VMEM((2, tok_rows, 128), f32),
            pltpu.VMEM((2, tok_rows, 128), f32),
            pltpu.VMEM((tok_rows, width), f32),
            pltpu.SemaphoreType.DMA((3,)),
            pltpu.SemaphoreType.DMA((2,)),
            pltpu.SemaphoreType.DMA((2,)),
        ]
        + lines,
        compiler_params=pltpu.CompilerParams(
            collective_id=0, has_side_effects=True, vmem_limit_bytes=60 * 1024 * 1024
        ),
    )(
        tokens,
        gain_in[None, :],
        gain_out[None, :],
        expert_ids.T,
        route_weight.T,
        gate_weight,
        up_weight,
        down_weight,
    )


def solution(mesh):
    in_specs = (
        P(("grp", "ep"), "tp"),
        P(),
        P(),
        P(("grp", "ep"), None),
        P(("grp", "ep"), None),
        P("ep", None, "tp"),
        P("ep", None, "tp"),
        P("ep", "tp", None),
    )
    out_specs = P(("grp", "ep"), "tp")
    return jax.shard_map(layer, mesh=mesh, in_specs=in_specs, out_specs=out_specs, check_vma=False)
```

```python
import functools

import jax
import jax.numpy as jnp
from jax import lax
from jax.experimental import pallas as pl
from jax.experimental.pallas import tpu as pltpu
from jax.sharding import PartitionSpec as P

norm_eps = 1e-06


def plain(
    tokens, gain_in, gain_out, expert_ids, route_weight, gate_weight, up_weight, down_weight
):
    tok_rows, half_width = tokens.shape
    full_width = 2 * half_width
    expert_count = lax.axis_size("ep") // 2
    picks = expert_ids.shape[1]
    capacity = tok_rows * picks * 3 // (2 * expert_count)
    own_cols = lax.axis_index("tp") * half_width
    own_float = tokens.astype(jnp.float32)
    squares = lax.psum(jnp.sum(own_float * own_float, axis=1), "tp")
    factor = lax.rsqrt(squares / full_width + norm_eps)[:, None]
    own_gain = lax.dynamic_slice_in_dim(gain_in, own_cols, half_width)
    normed = (own_float * factor * own_gain).astype(jnp.bfloat16)
    sent_width = normed.shape[1]
    flat_ids = expert_ids.reshape(-1)
    onehot = (flat_ids[:, None] == jnp.arange(expert_count, dtype=jnp.int32)[None, :]).astype(
        jnp.int32
    )
    before = jnp.cumsum(onehot, axis=0) - onehot
    targets = flat_ids * capacity + jnp.sum(before * onehot, axis=1)
    per_token = targets.reshape(tok_rows, picks)
    slot_rows = jnp.arange(expert_count * capacity, dtype=jnp.int32)[:, None]
    placing = jnp.zeros((expert_count * capacity, tok_rows), jnp.bfloat16)
    for which in range(picks):
        placing = placing + (slot_rows == per_token[None, :, which]).astype(jnp.bfloat16)
    packed = jnp.dot(placing, normed, preferred_element_type=jnp.float32).astype(jnp.bfloat16)
    stacked = packed.reshape(expert_count, 1, capacity, sent_width)
    outgoing = jnp.broadcast_to(stacked, (expert_count, 2, capacity, sent_width)).reshape(
        2 * expert_count, capacity, sent_width
    )
    arrived = lax.all_to_all(outgoing, "ep", split_axis=0, concat_axis=0, tiled=True)
    arrived = lax.all_gather(arrived, "tp", axis=2, tiled=True)
    sources = arrived.shape[0]
    gathered = arrived.reshape(sources * capacity, full_width)
    gate_pre = jnp.dot(gathered, gate_weight[0], preferred_element_type=jnp.float32)
    up_pre = jnp.dot(gathered, up_weight[0], preferred_element_type=jnp.float32)
    hidden = (jax.nn.silu(gate_pre) * up_pre).astype(jnp.bfloat16)
    partial_value = jnp.dot(hidden, down_weight[0], preferred_element_type=jnp.float32).astype(
        jnp.bfloat16
    )
    partial_value = partial_value.reshape(sources, capacity, full_width)
    half_sum = lax.psum_scatter(partial_value, "tp", scatter_dimension=2, tiled=True).astype(
        jnp.float32
    )
    returned = lax.all_to_all(
        half_sum.astype(jnp.bfloat16), "ep", split_axis=0, concat_axis=0, tiled=True
    )
    merged = jnp.sum(
        returned.reshape(expert_count, 2, capacity, half_width).astype(jnp.float32), axis=1
    )
    merged = merged.reshape(expert_count * capacity, half_width)
    picked = jnp.take(merged, targets, axis=0).reshape(tok_rows, picks, half_width)
    routed = jnp.sum(picked * route_weight[:, :, None], axis=1)
    squares_out = lax.psum(jnp.sum(routed * routed, axis=1), "tp")
    factor_out = lax.rsqrt(squares_out / full_width + norm_eps)[:, None]
    own_gain_out = lax.dynamic_slice_in_dim(gain_out, own_cols, half_width)
    return (routed * factor_out * own_gain_out).astype(jnp.bfloat16)


MESH = pl.DeviceIdType.MESH
pieces = 2


def fused(
    experts,
    cap,
    tok_ref,
    gain_in_ref,
    gain_out_ref,
    ids_ref,
    route_ref,
    gate_hbm,
    up_hbm,
    down_hbm,
    out_ref,
    packed,
    rows,
    parts,
    peer_parts,
    kept,
    crossing,
    crossed,
    leaving,
    home,
    gate_up,
    down,
    sums,
    peer_sums,
    total,
    w_sem,
    sq_send,
    sq_recv,
    line_send,
    line_recv,
    core_send,
    core_recv,
    pair_send,
    pair_recv,
    relay_send,
    relay_recv,
    part_send,
    part_recv,
    cross_send,
    cross_recv,
    home_send,
    home_recv,
):
    tok_rows, width = tok_ref.shape
    hidden_width = down.shape[0]
    place = lax.axis_index("ep")
    core = lax.axis_index("tp")
    half = place % 2
    mine = place // 2
    partner = place + 1 - 2 * half
    other = 1 - core
    own_cols = pl.ds(pl.multiple_of(core * width, 128), width)
    other_cols = pl.ds(pl.multiple_of(other * width, 128), width)

    piece = width // pieces

    def cut(s):
        return pl.ds(s * piece, piece)

    def of_core(which, s):
        return pl.ds(pl.multiple_of(which * width + s * piece, 128), piece)

    def on_line(step):
        return 2 * ((mine + step) % experts) + half

    loads = [
        pltpu.make_async_copy(gate_hbm.at[0], gate_up.at[:, pl.ds(0, hidden_width)], w_sem.at[0]),
        pltpu.make_async_copy(
            up_hbm.at[0], gate_up.at[:, pl.ds(hidden_width, hidden_width)], w_sem.at[1]
        ),
        pltpu.make_async_copy(down_hbm.at[0], down, w_sem.at[2]),
    ]
    barrier = pltpu.get_barrier_semaphore()
    pl.semaphore_signal(barrier, inc=1, device_id={"tp": other}, device_id_type=MESH)
    pl.semaphore_signal(barrier, inc=1, device_id={"ep": partner}, device_id_type=MESH)
    for step in range(1, experts):
        pl.semaphore_signal(barrier, inc=1, device_id={"ep": on_line(step)}, device_id_type=MESH)
    for load in loads:
        load.start()

    def remote(source, target, send, recv, device):
        return pltpu.make_async_remote_copy(
            src_ref=source,
            dst_ref=target,
            send_sem=send,
            recv_sem=recv,
            device_id=device,
            device_id_type=MESH,
        )

    def sum_copy(which):
        return remote(
            sums.at[which], peer_sums.at[which], sq_send.at[which], sq_recv.at[which], {"tp": other}
        )

    def line_copy(step, s):
        back = experts - step
        return remote(
            packed.at[step, :, cut(s)],
            rows.at[back, 0, :, of_core(core, s)],
            line_send.at[back * pieces + s],
            line_recv.at[back * pieces + s],
            {"ep": on_line(step)},
        )

    def core_copy(d, s, which=core):
        view, sem = rows.at[d, 0, :, of_core(which, s)], d * pieces + s
        return remote(view, view, core_send.at[sem], core_recv.at[sem], {"tp": other})

    def pair_copy(d, s):
        return remote(
            rows.at[d, 0, :, of_core(core, s)],
            rows.at[d, 1, :, of_core(core, s)],
            pair_send.at[d * pieces + s],
            pair_recv.at[d * pieces + s],
            {"ep": partner},
        )

    def relay_copy(d, s, which=core):
        view, sem = rows.at[d, 1, :, of_core(which, s)], d * pieces + s
        return remote(view, view, relay_send.at[sem], relay_recv.at[sem], {"tp": other})

    def part_copy(d):
        return remote(
            parts.at[d, :, :, other_cols],
            peer_parts.at[d],
            part_send.at[d],
            part_recv.at[d],
            {"tp": other},
        )

    def cross_copy(d, s):
        sem = d * pieces + s
        return remote(
            crossing.at[d, :, cut(s)],
            crossed.at[d, :, cut(s)],
            cross_send.at[sem],
            cross_recv.at[sem],
            {"ep": partner},
        )

    def home_copy(d, s):
        back = experts - d
        sem = back * pieces + s
        return remote(
            leaving.at[d, :, cut(s)],
            home.at[back, :, cut(s)],
            home_send.at[sem],
            home_recv.at[sem],
            {"ep": on_line(d)},
        )

    own_float = tok_ref[...].astype(jnp.float32)
    sums[0] = jnp.broadcast_to(
        jnp.sum(own_float * own_float, axis=1, keepdims=True), (tok_rows, 128)
    )
    pl.semaphore_wait(barrier, experts + 1)
    sum_copy(0).start()

    lead = max(8, experts)
    names = lax.broadcasted_iota(jnp.int32, (lead, tok_rows), 0)
    first = names == ids_ref[0:1, :]
    second = names == ids_ref[1:2, :]
    either = (first.astype(jnp.float32) + second.astype(jnp.float32)).astype(jnp.bfloat16)
    earlier = (
        lax.broadcasted_iota(jnp.int32, (tok_rows, tok_rows), 0)
        < lax.broadcasted_iota(jnp.int32, (tok_rows, tok_rows), 1)
    ).astype(jnp.float32).astype(jnp.bfloat16)
    before = jnp.dot(either, earlier, preferred_element_type=jnp.float32)
    slot_one = jnp.sum(jnp.where(first, before, 0.0), axis=0, keepdims=True).astype(jnp.int32)
    slot_two = jnp.sum(jnp.where(second, before, 0.0), axis=0, keepdims=True).astype(jnp.int32)
    target_one = ids_ref[0:1, :] * cap + slot_one
    target_two = ids_ref[1:2, :] * cap + slot_two
    slot_rows = lax.broadcasted_iota(jnp.int32, (cap, tok_rows), 0)

    def hits(step):
        base = ((mine + step) % experts) * cap
        return slot_rows + base == target_one, slot_rows + base == target_two

    sum_copy(0).wait_recv()
    squares = sums[0] + peer_sums[0]
    factor = lax.rsqrt(squares[:, 0:1] / (2 * width) + norm_eps)
    normed = (own_float * factor * gain_in_ref[:, own_cols]).astype(jnp.bfloat16)

    def pack(step):
        one, two = hits(step)
        placing = (one.astype(jnp.float32) + two.astype(jnp.float32)).astype(jnp.bfloat16)
        return jnp.dot(placing, normed, preferred_element_type=jnp.float32).astype(jnp.bfloat16)

    rows[0, 0, :, own_cols] = pack(0)
    for s in range(pieces):
        pair_copy(0, s).start()
        core_copy(0, s).start()
    for step in range(experts - 1, 0, -1):
        packed[step] = pack(step)
        for s in range(pieces):
            line_copy(step, s).start()

    def relay_line(d):
        for s in range(pieces):
            line_copy(experts - d, s).wait_recv()
            pair_copy(d, s).start()
            core_copy(d, s).start()

    def relay_pair(d):
        for s in range(pieces):
            pair_copy(d, s).wait_recv()
            relay_copy(d, s).start()

    def compute(d):
        for s in range(pieces):
            core_copy(d, s, other).wait_recv()
            relay_copy(d, s, other).wait_recv()
        block = rows[d].reshape(2 * cap, 2 * width)
        pre = jnp.dot(block, gate_up[...], preferred_element_type=jnp.float32)
        gate_pre = pre[:, :hidden_width]
        hidden = (gate_pre / (1.0 + jnp.exp(-gate_pre)) * pre[:, hidden_width:]).astype(
            jnp.bfloat16
        )
        partial = jnp.dot(hidden, down[...], preferred_element_type=jnp.float32)
        parts[d] = partial.astype(jnp.bfloat16).reshape(2, cap, 2 * width)
        part_copy(d).start()

    def cross(d):
        part_copy(d).wait_recv()
        for s in range(pieces):
            crossing[d, :, cut(s)] = (
                parts[d, 1, :, of_core(core, s)].astype(jnp.float32)
                + peer_parts[d, 1, :, cut(s)].astype(jnp.float32)
            ).astype(jnp.bfloat16)
            cross_copy(d, s).start()
        kept[d] = parts[d, 0, :, own_cols].astype(jnp.float32) + peer_parts[d, 0].astype(
            jnp.float32
        )

    def meet(d, s):
        cross_copy(d, s).wait_recv()
        return (kept[d, :, cut(s)] + crossed[d, :, cut(s)].astype(jnp.float32)).astype(
            jnp.bfloat16
        )

    def keep_own():
        for s in range(pieces):
            home[0, :, cut(s)] = meet(0, s)

    def send_home(d):
        for s in range(pieces):
            leaving[d, :, cut(s)] = meet(d, s)
            home_copy(d, s).start()

    relay_pair(0)
    for load in loads:
        load.wait()

    def step_of(d, carry):
        @pl.when(d + 1 < experts)
        def _():
            relay_line(d + 1)

        compute(d)
        cross(d)

        @pl.when(d == 1)
        def _():
            keep_own()

        @pl.when(d > 1)
        def _():
            send_home(d - 1)

        @pl.when(d + 1 < experts)
        def _():
            relay_pair(d + 1)

        return carry

    lax.fori_loop(0, experts, step_of, 0)
    send_home(experts - 1)

    def weights_of(step):
        one, two = hits(step)
        mix = jnp.where(one, route_ref[0:1, :], 0.0) + jnp.where(two, route_ref[1:2, :], 0.0)
        high = mix.astype(jnp.bfloat16)
        return high, (mix - high.astype(jnp.float32)).astype(jnp.bfloat16)

    def combine(step, s, high, low):
        dims = (((0,), (0,)), ((), ()))
        values = home[step, :, cut(s)]
        return lax.dot_general(
            high, values, dims, preferred_element_type=jnp.float32
        ) + lax.dot_general(low, values, dims, preferred_element_type=jnp.float32)

    mixes = weights_of(0)
    for s in range(pieces):
        total[:, cut(s)] = combine(0, s, *mixes)
    for step in range(experts - 1, 0, -1):
        mixes = weights_of(step)
        for s in range(pieces):
            home_copy(experts - step, s).wait_recv()
            total[:, cut(s)] += combine(step, s, *mixes)
    routed = total[...]
    sums[1] = jnp.broadcast_to(jnp.sum(routed * routed, axis=1, keepdims=True), (tok_rows, 128))
    sum_copy(1).start()
    sum_copy(1).wait_recv()
    squares_out = sums[1] + peer_sums[1]
    factor_out = lax.rsqrt(squares_out[:, 0:1] / (2 * width) + norm_eps)
    out_ref[...] = (total[...] * factor_out * gain_out_ref[:, own_cols]).astype(jnp.bfloat16)

    sum_copy(0).wait_send()
    sum_copy(1).wait_send()

    def drain(d, carry):
        for s in range(pieces):
            core_copy(d, s).wait_send()
            pair_copy(d, s).wait_send()
            relay_copy(d, s).wait_send()
            cross_copy(d, s).wait_send()
        part_copy(d).wait_send()

        @pl.when(d > 0)
        def _():
            for s in range(pieces):
                line_copy(d, s).wait_send()
                home_copy(d, s).wait_send()

        return carry

    lax.fori_loop(0, experts, drain, 0)


def layer(
    tokens, gain_in, gain_out, expert_ids, route_weight, gate_weight, up_weight, down_weight
):
    tok_rows, width = tokens.shape
    experts = lax.axis_size("ep") // 2
    picks = expert_ids.shape[1]
    cap = tok_rows * picks * 3 // (2 * experts)
    hidden_width = gate_weight.shape[2]
    if picks != 2 or experts < 2 or cap % 16 or width % (128 * pieces) or hidden_width % 128:
        return plain(
            tokens, gain_in, gain_out, expert_ids, route_weight, gate_weight, up_weight, down_weight
        )
    vmem = pl.BlockSpec(memory_space=pltpu.VMEM)
    hbm = pl.BlockSpec(memory_space=pl.ANY)
    bf16, f32 = jnp.bfloat16, jnp.float32
    lines = [pltpu.SemaphoreType.DMA((experts * pieces,))] * 14
    return pl.pallas_call(
        functools.partial(fused, experts, cap),
        out_shape=jax.ShapeDtypeStruct((tok_rows, width), bf16),
        in_specs=[vmem] * 5 + [hbm] * 3,
        out_specs=vmem,
        scratch_shapes=[
            pltpu.VMEM((experts, cap, width), bf16),
            pltpu.VMEM((experts, 2, cap, 2 * width), bf16),
            pltpu.VMEM((experts, 2, cap, 2 * width), bf16),
            pltpu.VMEM((experts, 2, cap, width), bf16),
            pltpu.VMEM((experts, cap, width), f32),
            pltpu.VMEM((experts, cap, width), bf16),
            pltpu.VMEM((experts, cap, width), bf16),
            pltpu.VMEM((experts, cap, width), bf16),
            pltpu.VMEM((experts, cap, width), bf16),
            pltpu.VMEM((2 * width, 2 * hidden_width), bf16),
            pltpu.VMEM((hidden_width, 2 * width), bf16),
            pltpu.VMEM((2, tok_rows, 128), f32),
            pltpu.VMEM((2, tok_rows, 128), f32),
            pltpu.VMEM((tok_rows, width), f32),
            pltpu.SemaphoreType.DMA((3,)),
            pltpu.SemaphoreType.DMA((2,)),
            pltpu.SemaphoreType.DMA((2,)),
        ]
        + lines,
        compiler_params=pltpu.CompilerParams(
            collective_id=0, has_side_effects=True, vmem_limit_bytes=60 * 1024 * 1024
        ),
    )(
        tokens,
        gain_in[None, :],
        gain_out[None, :],
        expert_ids.T,
        route_weight.T,
        gate_weight,
        up_weight,
        down_weight,
    )


def solution(mesh):
    in_specs = (
        P(("grp", "ep"), "tp"),
        P(),
        P(),
        P(("grp", "ep"), None),
        P(("grp", "ep"), None),
        P("ep", None, "tp"),
        P("ep", None, "tp"),
        P("ep", "tp", None),
    )
    out_specs = P(("grp", "ep"), "tp")
    return jax.shard_map(layer, mesh=mesh, in_specs=in_specs, out_specs=out_specs, check_vma=False)
```
